256 devices in a mesh: ep: 64 (over z, y, core), tp: 4 (over x).
Axes of the slice: x: 4, y: 4, z: 8, core: 2. Of those that a mesh axis runs over, the one named last changes fastest.
Arguments:
- tokens: bfloat16 [16384, 2048], P('ep'), may hold values from -6 to 6
- norm_gain: float32 [2048], replicated, may hold values from 0.1 to 1.9
- expert_ids: int32 [16384, 2], P('ep'), may hold values from 0 to 31, all different within a row; in each aligned block of 256 rows (0 to 255, 256 to 511, ...) at most 20 rows name the same one
- route_weight: float32 [16384, 2], P('ep'), may hold values from 0.2 to 1
- w_gate: bfloat16 [64, 2048, 3584], P('ep', None, 'tp'), may hold values from -0.125 to 0.125
- w_up: bfloat16 [64, 2048, 3584], P('ep', None, 'tp'), may hold values from -0.125 to 0.125
- w_down: bfloat16 [64, 3584, 2048], P('ep', 'tp'), may hold values from -0.0625 to 0.0625
Outputs:
- mixed: bfloat16 [16384, 2048], P('ep', 'tp')
The draws below stay inside these ranges and needn't reach their ends.
Inputs may be any that keep to these rules, and one draw needn't show every extreme that they name: `expert_ids`: A token names 2 different experts. In each aligned block of 256 tokens (the tokens of one index of ep) no expert is named by more than 20 tokens, a bound that some block reaches.
All inputs are finite; a program needn't handle non-finite values.
Results may differ from the reference program's by a relative error of at most 0.014.
Values may be sent and summed in bfloat16 or wider, within the bound.
No kernel may reach another device: no remote copies, remote signals or barrier semaphores. Data moves between devices by JAX's collectives and lax.ppermute only.
A program may use at most 128 MiB of HBM per device.

```python
import math
import jax
import jax.numpy as jnp
import numpy as np
from jax import lax

D = 2048
FF = 7168
TOP = 2
HALVES = 2
TOK_DEV = 256
EXPERTS = 32
HALF_FF = 3584
BLOCK_H = 896
CAP = 20
TOKENS = 16384
N_EP = 64
N_TP = 4


def steps_of(key, dims, pieces, smallest, top_value):
    loudness = 1.0
    for axis_at, shards_of in pieces:
        heights = jax.random.uniform(jax.random.fold_in(jax.random.fold_in(key, 6), axis_at), (shards_of,), jnp.float32, smallest / len(pieces), top_value / len(pieces))
        loudness = loudness * jnp.repeat(jnp.exp(heights), dims[axis_at] // shards_of).reshape((-1,) + (1,) * (len(dims) - 1 - axis_at))
    return loudness


def assign_block(rng, own, number, rows, number_of, top, bound, slope):
    sequence = jax.random.permutation(rng, number_of)
    packed, ordinary = shares(number_of, rows * top, bound, slope, True), shares(number_of, rows * top, bound, slope, False)
    places = jnp.arange(number_of)

    def named(tallies, offset_by):
        used = int((tallies > 0).sum())
        fixed = max(1, used // 4)
        shifted = fixed + (places - fixed + offset_by * (used - fixed)) % max(1, number_of - fixed)
        return jnp.zeros((number_of,), jnp.int32).at[sequence[jnp.where(places < fixed, places, shifted)]].set(jnp.asarray(tallies, jnp.int32))

    tallies = jnp.where(number % 4 == 0, named(packed, number // 4), named(ordinary, number - number // 4 - 1))
    mixed = jax.random.permutation(jax.random.fold_in(own, 3), number_of)
    donor, receiver = mixed[0:number_of // 2 * 2:2], mixed[1:number_of // 2 * 2:2]
    room = jnp.minimum(tallies[donor] - 1, bound - tallies[receiver]) // 2
    room = jnp.where((donor == sequence[0]) | (receiver == sequence[0]) | (tallies[receiver] == 0), 0, jnp.maximum(room, 0))
    shifted = jax.random.randint(jax.random.fold_in(own, 4), (number_of // 2,), 0, 1 << 20) % (room + 1)
    tallies = tallies.at[donor].add(-shifted).at[receiver].add(shifted)
    members = jnp.searchsorted(jnp.cumsum(tallies), jnp.arange(rows * top), side="right").astype(jnp.int32)
    table = members.reshape(top, rows).T
    table = table[jax.random.permutation(jax.random.fold_in(own, 1), rows)]
    offset_by = jax.random.randint(jax.random.fold_in(own, 2), (rows, 1), 0, top)
    return jnp.take_along_axis(table, (jnp.arange(top)[None, :] + offset_by) % top, axis=1)


def shares(count, total, reach, skew, full):
    portions = [(1 << 20) // math.isqrt(grade ** skew) + 1 for grade in range(1, count + 1)]
    largest = reach if full else min(reach, max(-(-total // count), total * portions[0] // sum(portions)))
    least = 1 if total - largest >= count - 1 else 0
    holding, surplus = [largest] + [least] * (count - 1), total - largest - least * (count - 1)
    while surplus > 0:
        movable = [i for i in range(1, count) if holding[i] < largest] or [i for i in range(1, count) if holding[i] < reach]
        mass, remaining = sum([portions[i] for i in movable]), surplus
        for i in movable:
            addition = min(reach - holding[i], max(1, remaining * portions[i] // mass), surplus)
            holding[i] = holding[i] + addition
            surplus = surplus - addition
    return np.array(holding)


def normal_values(own_key, extent, scale, most, split=(), kind=jnp.bfloat16):
    gain = steps_of(own_key, extent, split, -0.22, 0.18) if split else 1.0
    entries = jax.random.normal(own_key, extent, jnp.float32) * scale * gain
    return jnp.minimum(jnp.maximum(entries, -most), most).astype(kind)


def setup_inputs(seed: int = 0) -> dict:
    key_list = jax.random.split(jax.random.key(seed), 8)
    tokens = normal_values(key_list[0], (TOKENS, D), 1.0, 6.0, ((0, 64),))
    norm_gain = jnp.clip(1.0 + 0.18 * jax.random.normal(key_list[1], (D,), jnp.float32), 0.1, 1.9)
    expert_ids_keys = jax.random.split(jax.random.fold_in(key_list[2], 1), TOKENS // TOK_DEV)
    expert_ids_turns = jax.random.permutation(jax.random.fold_in(key_list[2], 3), TOKENS // TOK_DEV)
    expert_ids = jax.vmap(lambda own, number: assign_block(jax.random.fold_in(key_list[2], 2), own, number, TOK_DEV, EXPERTS, TOP, CAP, 1))(expert_ids_keys, expert_ids_turns).reshape((TOKENS, TOP))
    route_weight = jnp.clip(0.2 + 0.8 * jax.random.uniform(key_list[3], (TOKENS, TOP), jnp.float32) ** steps_of(key_list[3], (TOKENS, TOP), ((0, 64),), -0.2, 0.2), 0.2, 1.0)
    w_gate = normal_values(key_list[4], (EXPERTS * HALVES, D, HALF_FF), D ** -0.5, 0.125, ((0, 64), (2, 4)))
    w_up = normal_values(key_list[5], (EXPERTS * HALVES, D, HALF_FF), D ** -0.5, 0.125, ((0, 64), (2, 4)))
    w_down = normal_values(key_list[6], (EXPERTS * HALVES, HALF_FF, D), FF ** -0.5, 0.0625, ((0, 64), (1, 4)))
    return {"tokens": tokens, "norm_gain": norm_gain, "expert_ids": expert_ids, "route_weight": route_weight, "w_gate": w_gate, "w_up": w_up, "w_down": w_down}


EPSILON = 1e-05

def layer_normed(tokens, norm_gain):
    values = tokens.astype(jnp.float32)
    center = values - lax.optimization_barrier(jnp.mean(values, axis=-1, keepdims=True))
    spread = lax.optimization_barrier(jnp.mean(center * center, axis=-1, keepdims=True))
    return (center * lax.rsqrt(spread + EPSILON) * norm_gain).astype(jnp.bfloat16)

def slot_numbers(chosen, experts):
    onehot = (chosen[..., None] == jnp.arange(experts, dtype=jnp.int32)).astype(jnp.int32)
    before = jnp.cumsum(onehot, axis=1) - onehot
    return lax.optimization_barrier(jnp.sum(before * onehot, axis=-1)).astype(jnp.int32)

def reference(tokens, norm_gain, expert_ids, route_weight, w_gate, w_up, w_down):
    normed = layer_normed(tokens, norm_gain)
    padded = jnp.concatenate([normed, jnp.zeros((1, D), jnp.bfloat16)], axis=0)
    pair_count = TOK_DEV * TOP
    slots = slot_numbers(expert_ids.reshape(N_EP, pair_count), EXPERTS).reshape(-1)
    flat_expert = expert_ids.reshape(-1).astype(jnp.int32)
    index = jnp.arange(TOKENS * TOP, dtype=jnp.int32)
    source = index // pair_count
    owner = index // TOP
    place = (flat_expert * N_EP + source) * CAP + slots
    table = jnp.full((EXPERTS * N_EP * CAP,), TOKENS, jnp.int32).at[place].set(owner)
    table = table.reshape(EXPERTS, N_EP * CAP)

    def one_expert(expert):
        rows = padded[table[expert]]
        total = jnp.zeros((N_EP * CAP, D), jnp.float32)
        for half in range(HALVES):
            which = expert * HALVES + half
            gate = jnp.dot(rows, w_gate[which], preferred_element_type=jnp.float32)
            up = jnp.dot(rows, w_up[which], preferred_element_type=jnp.float32)
            hidden = (jax.nn.silu(gate) * up).astype(jnp.bfloat16)
            blocks = hidden.reshape(N_EP * CAP, N_TP, BLOCK_H).astype(jnp.float32)
            down = w_down[which].reshape(N_TP, BLOCK_H, D).astype(jnp.float32)
            block_out = jnp.einsum('rnb,nbd->nrd', blocks, down).astype(jnp.bfloat16)
            half_out = lax.optimization_barrier(jnp.sum(block_out.astype(jnp.float32), axis=0)).astype(jnp.bfloat16)
            total = total + half_out.astype(jnp.float32)
        return total
    results = lax.map(one_expert, jnp.arange(EXPERTS, dtype=jnp.int32))
    merged = results.reshape(EXPERTS * N_EP * CAP, D)
    picked = merged[place].reshape(TOKENS, TOP, D)
    return lax.optimization_barrier(jnp.sum(route_weight[:, :, None] * picked, axis=1)).astype(jnp.bfloat16)
```

```python
import functools

import jax
import jax.numpy as jnp
from jax import lax
from jax.experimental import pallas as pl
from jax.experimental.pallas import tpu as pltpu
from jax.sharding import Mesh
from jax.sharding import PartitionSpec as P

EPSILON = 1e-05
EP = ("z", "y", "c")
CHUNKS = (16, 24)
NONE = -64.0
BF, F32 = jnp.bfloat16, jnp.float32
VMEM_LIMIT = 60 * 1024 * 1024


def whole(space=pltpu.VMEM):
    return pl.BlockSpec(memory_space=space)


def prep_kernel(sel, tok, gain, ids, weight, own, give):
    rows, width = tok.shape
    eighth = own.shape[1]
    values = tok[...].astype(F32)
    mean = jnp.sum(values, axis=1, keepdims=True) * (1.0 / width)
    center = values - mean
    spread = jnp.sum(center * center, axis=1, keepdims=True) * (1.0 / width)
    inverse = lax.rsqrt(spread + EPSILON)
    experts = (own.shape[0] - rows) // 3
    for at, out in ((0, own), (1, give)):
        columns = pl.ds(pl.multiple_of(sel[at] * eighth, eighth), eighth)
        part = tok[:, columns].astype(F32) - mean
        out[0:rows, :] = (part * inverse * gain[:, columns]).astype(BF)
    number = lax.broadcasted_iota(jnp.int32, (experts, rows), 0)
    first, second = number == ids[0:1, :], number == ids[1:2, :]
    named = jnp.where(first | second, 1.0, 0.0)
    earlier = lax.broadcasted_iota(jnp.int32, (rows, rows), 0) < lax.broadcasted_iota(jnp.int32, (rows, rows), 1)
    before = jnp.dot(named.astype(BF), jnp.where(earlier, 1.0, 0.0).astype(BF), preferred_element_type=F32)
    slot = jnp.where(named > 0, before, NONE).astype(BF)
    scale = jnp.where(first, weight[0:1, :], 0.0) + jnp.where(second, weight[1:2, :], 0.0)
    high = scale.astype(BF)
    low = (scale - high.astype(F32)).astype(BF)
    for out in (own, give):
        out[rows : rows + experts, :] = slot
        out[rows + experts : rows + 2 * experts, :] = high
        out[rows + 2 * experts :, :] = low


def slots_of(sel, own, sib, rows, experts, capacity):
    shift = (sel[2] * capacity).astype(F32)
    mine = own[rows : rows + experts, :].astype(F32) + shift
    other = sib[rows : rows + experts, :].astype(F32) + (capacity - shift)
    return jnp.concatenate([mine, other], axis=1)


def send_kernel(sel, own, sib, *rest, chunks, rows, experts, capacity):
    outs, picks = rest[: len(chunks)], rest[len(chunks) :]
    slots = slots_of(sel, own, sib, rows, experts, capacity)
    both = jnp.concatenate([own[0:rows, :], sib[0:rows, :]], axis=0)
    start = 0
    for size, out, pick in zip(chunks, outs, picks, strict=True):
        wanted = (lax.broadcasted_iota(jnp.int32, (size, 2 * rows), 0) + start).astype(F32)
        for e in range(0, experts, 2):
            pair = [jnp.where(slots[k : k + 1, :] == wanted, 1.0, 0.0) for k in (e, e + 1)]
            pick[e * size : (e + 2) * size, :] = jnp.concatenate(pair, axis=0).astype(BF)
        out[...] = jnp.dot(pick[...], both, preferred_element_type=F32).astype(BF)
        start += size


def mixer_kernel(sel, own, sib, *outs, chunks, rows, experts, capacity):
    slots = slots_of(sel, own, sib, rows, experts, capacity)
    for half in range(2):
        at = rows + experts * (1 + half)
        scale = jnp.concatenate([own[at : at + experts, :], sib[at : at + experts, :]], axis=1).astype(F32)
        start = 0
        for number, size in enumerate(chunks):
            out = outs[2 * number + half]
            wanted = (lax.broadcasted_iota(jnp.int32, (size, 2 * rows), 0) + start).astype(F32)
            group = 16
            for e in range(0, experts, group):
                block = [jnp.where(slots[k : k + 1, :] == wanted, scale[k : k + 1, :], 0.0) for k in range(e, e + group)]
                out[:, e * size : (e + group) * size] = jnp.concatenate(block, axis=0).T.astype(BF)
            start += size


def combine_kernel(*refs, count):
    own, give = refs[3 * count :]
    rows = own.shape[0]
    total = None
    for number in range(count):
        high, low, results = refs[3 * number : 3 * number + 3]
        for scale in (high, low):
            term = jnp.dot(scale[...], results[...], preferred_element_type=F32)
            total = term if total is None else total + term
    own[...] = total[:rows, :].astype(BF)
    give[...] = total[rows:, :].astype(BF)


def expert_kernel(sel, *refs, block):
    pieces, (wg, wu, wd), refs = refs[:8], refs[8:11], refs[11:]
    outs, (xs, gs, us, ds, sems) = refs[:8], refs[8:]
    eighth = pieces[0].shape[1]
    step = pl.program_id(0)

    def copies(kind):
        for k in range(8):
            here = pl.ds(k * eighth, eighth)
            source = pl.ds(pl.multiple_of(sel[3 + k] * eighth, eighth), eighth)
            target = pl.ds(pl.multiple_of(sel[11 + k] * eighth, eighth), eighth)
            if kind == 0:
                yield pltpu.make_async_copy(pieces[k], xs.at[:, here], sems.at[0, k])
            elif kind == 1:
                yield pltpu.make_async_copy(wg.at[0, source, :], gs.at[here, :], sems.at[1, k])
            elif kind == 2:
                yield pltpu.make_async_copy(wu.at[0, source, :], us.at[here, :], sems.at[2, k])
            else:
                yield pltpu.make_async_copy(wd.at[0, :, target], ds.at[:, here], sems.at[3, k])

    @pl.when(step == 0)
    def _():
        for kind in (1, 0, 2, 3):
            for copy in copies(kind):
                copy.start()
        for kind in (1, 0):
            for copy in copies(kind):
                copy.wait()

    rows = xs[pl.ds(pl.multiple_of(step * block, block), block), :]
    gate = jnp.dot(rows, gs[...], preferred_element_type=F32)

    @pl.when(step == 0)
    def _():
        for copy in copies(2):
            copy.wait()

    up = jnp.dot(rows, us[...], preferred_element_type=F32)
    hidden = (gate / (1.0 + jnp.exp(-gate)) * up).astype(BF)

    @pl.when(step == 0)
    def _():
        for copy in copies(3):
            copy.wait()

    for k in range(8):
        part = jnp.dot(hidden, ds[:, k * eighth : (k + 1) * eighth], preferred_element_type=F32)
        outs[k][...] = part.astype(BF)


def expert(sel, pieces, wg, wu, wd, block=256):
    rows, eighth = pieces[0].shape
    _, width, hidden = wg.shape
    return pl.pallas_call(
        functools.partial(expert_kernel, block=block),
        grid=(rows // block,),
        in_specs=[whole(pltpu.SMEM)] + [whole(pltpu.HBM)] * 11,
        out_specs=[pl.BlockSpec((block, eighth), lambda i: (i, 0))] * 8,
        out_shape=[jax.ShapeDtypeStruct((rows, eighth), BF)] * 8,
        scratch_shapes=[
            pltpu.VMEM((rows, width), BF),
            pltpu.VMEM((width, hidden), BF),
            pltpu.VMEM((width, hidden), BF),
            pltpu.VMEM((hidden, width), BF),
            pltpu.SemaphoreType.DMA((4, 8)),
        ],
        compiler_params=pltpu.CompilerParams(vmem_limit_bytes=VMEM_LIMIT, dimension_semantics=("arbitrary",)),
        cost_estimate=pl.CostEstimate(
            flops=6 * rows * width * hidden,
            bytes_accessed=6 * width * hidden + 4 * rows * width,
            transcendentals=2 * rows * hidden,
        ),
        name="expert",
    )(sel, *pieces, wg, wu, wd)


def small(kernel, outs, scratch=(), flops=1 << 28, name=None):
    def call(sel, *args):
        return pl.pallas_call(
            kernel,
            in_specs=[whole(pltpu.SMEM)] * (sel is not None) + [whole()] * len(args),
            out_specs=[whole()] * len(outs),
            out_shape=outs,
            scratch_shapes=scratch,
            compiler_params=pltpu.CompilerParams(vmem_limit_bytes=32 * 1024 * 1024),
            cost_estimate=pl.CostEstimate(flops=flops, bytes_accessed=4 << 20, transcendentals=0),
            name=name,
        )(*([sel] * (sel is not None)), *args)

    return call


def added(*arrays):
    return sum(a.astype(F32) for a in arrays).astype(BF)


def body(tokens, norm_gain, expert_ids, route_weight, w_gate, w_up, w_down):
    rows, width = tokens.shape
    experts = lax.axis_size("z") * lax.axis_size("y")
    across = lax.axis_size("x")
    eighth = width // (2 * across)
    capacity = sum(CHUNKS) // 2
    x, c = lax.axis_index("x"), lax.axis_index("c")

    def swap(value):
        return lax.ppermute(value, "c", [(0, 1), (1, 0)])

    def shift(value, by):
        return lax.ppermute(value, "x", [(i, (i + by) % across) for i in range(across)])

    def exchange(value):
        parts = value.reshape(experts, value.shape[0] // experts, eighth)
        return lax.all_to_all(parts, ("z", "y"), 0, 0, tiled=True).reshape(value.shape)

    near = [(x + by) % across for by in (0, 1, 3, 2)]
    sel = jnp.stack(
        [2 * x + c, 2 * x + 1 - c, c]
        + [2 * near[k] + h for h in (c, 1 - c) for k in (0, 2, 1, 3)]
        + [2 * near[k] + h for h in (c, 1 - c) for k in (0, 1, 2, 3)]
    ).astype(jnp.int32)

    meta = jax.ShapeDtypeStruct((rows + 3 * experts, eighth), BF)
    own, give = small(prep_kernel, [meta, meta], name="prep")(
        sel, tokens, norm_gain.reshape(1, width), expert_ids.T, route_weight.T
    )
    sib = swap(give)
    sizes = dict(chunks=CHUNKS, rows=rows, experts=experts, capacity=capacity)
    sends = small(
        functools.partial(send_kernel, **sizes),
        [jax.ShapeDtypeStruct((experts * s, eighth), BF) for s in CHUNKS],
        [pltpu.VMEM((experts * s, 2 * rows), BF) for s in CHUNKS],
        name="send",
    )(sel, own, sib)
    mixers = small(
        functools.partial(mixer_kernel, **sizes),
        [jax.ShapeDtypeStruct((2 * rows, experts * s), BF) for s in CHUNKS for _ in range(2)],
        flops=1 << 31,
        name="mixer",
    )(sel, own, sib)

    operands = []
    for number, send in enumerate(sends):
        way = 1 if number % 2 == 0 else -1
        mine = exchange(send)
        left = shift(mine, 1)
        right = shift(mine, -1)
        far = shift(left if way == 1 else right, way)
        held = [mine, left, right, far]
        pieces = held + [swap(h) for h in held]
        outs = expert(sel, pieces, w_gate, w_up, w_down)
        keep, give = outs[:4], outs[4:]
        parts = [added(k, swap(g)) for k, g in zip(keep, give, strict=True)]
        passed = shift(parts[3], way)
        near_by = 1 if way == 1 else 2
        relayed = shift(added(parts[near_by], passed), way)
        direct = shift(parts[3 - near_by], -way)
        result = exchange(added(parts[0], relayed, direct))
        operands += [mixers[2 * number], mixers[2 * number + 1], result]
    half = jax.ShapeDtypeStruct((rows, eighth), BF)
    final, give = small(functools.partial(combine_kernel, count=len(CHUNKS)), [half, half], name="combine")(None, *operands)
    other = swap(give)
    first = jnp.where(c == 0, final, other)
    second = jnp.where(c == 0, other, final)
    return jnp.concatenate([first, second], axis=1)


def solution(mesh):
    finer = Mesh(mesh.devices.reshape(8, 4, 2, mesh.shape["tp"]), ("z", "y", "c", "x"))
    in_specs = (
        P(EP, None),
        P(),
        P(EP, None),
        P(EP, None),
        P(EP, None, "x"),
        P(EP, None, "x"),
        P(EP, "x", None),
    )
    return jax.shard_map(body, mesh=finer, in_specs=in_specs, out_specs=P(EP, "x"), check_vma=False)
```

```python
import functools

import jax
import jax.numpy as jnp
from jax import lax
from jax.experimental import pallas as pl
from jax.experimental.pallas import tpu as pltpu
from jax.sharding import Mesh
from jax.sharding import PartitionSpec as P


EPSILON = 1e-05
EP = ("z", "y", "c")
CAP, MAIN, REST = 20, 16, 4
LANES = 128
NONE = -64.0
BF, F32 = jnp.bfloat16, jnp.float32
MIB = 1024 * 1024


dot = functools.partial(jnp.dot, preferred_element_type=F32)


def whole(space=pltpu.VMEM):
    return pl.BlockSpec(memory_space=space)


def iota(shape, dim):
    return lax.broadcasted_iota(jnp.int32, shape, dim)


def moved(groups, k, dtype=BF):
    plain = (REST * groups, MAIN * groups)
    group_of = iota(plain, 0) // REST == iota(plain, 1) // MAIN
    same = iota(plain, 1) % MAIN == iota(plain, 0) % REST + k * REST
    return jnp.where(group_of & same, 1.0, 0.0).astype(dtype)


def packed(main, rest, write):
    groups, parts = main.shape[0] // MAIN, main.shape[1] // LANES
    last = None
    for k in range(parts):
        here = slice(k * LANES, (k + 1) * LANES)
        write(slice(k * MAIN, (k + 1) * MAIN), main[:, here].reshape(groups, MAIN, LANES))
        term = lax.dot_general(moved(groups, k), rest[:, here], (((0,), (0,)), ((), ())), preferred_element_type=F32)
        last = term if last is None else last + term
    write(slice(parts * MAIN, parts * (MAIN + REST)), last.astype(BF).reshape(groups, MAIN, LANES))


def unpacked(read, groups, parts, write):
    last = read(slice(parts * MAIN, parts * (MAIN + REST))).reshape(groups * MAIN, LANES)
    for k in range(parts):
        here = slice(k * LANES, (k + 1) * LANES)
        write(slice(0, groups * MAIN), here, read(slice(k * MAIN, (k + 1) * MAIN)).reshape(groups * MAIN, LANES))
        write(slice(groups * MAIN, groups * CAP), here, dot(moved(groups, k), last).astype(BF))


def rows_of_experts(experts, flip):
    rows = experts * CAP
    row, expert = (iota((rows, experts), 0), iota((rows, experts), 1))
    first = experts * MAIN
    owner = jnp.where(row < first, row // MAIN, (row - first) // REST)
    spread = jnp.where(owner == expert, 1.0, 0.0).astype(BF)
    shape, dim = ((1, rows), 1) if flip else ((rows, 1), 0)
    at = iota(shape, dim)
    slot = jnp.where(at < first, at % MAIN, MAIN + (at - first) % REST).astype(F32)
    return spread, slot


def prep_kernel(sel, tokens, gain_hbm, ids_hbm, weight_hbm, message, slots, high, low, tok, gain, ids, weight, sems):
    copies = [
        pltpu.make_async_copy(source, target, sems.at[n])
        for n, (source, target) in enumerate(
            ((ids_hbm, ids), (tokens, tok), (gain_hbm, gain), (weight_hbm, weight))
        )
    ]
    for copy in copies:
        copy.start()
    rows, width = tok.shape
    experts = slots.shape[0]
    quarter = message.shape[1] // CAP * LANES
    copies[0].wait()
    number = iota((experts, rows), 0)
    first, second = number == ids[0:1, :], number == ids[1:2, :]
    named = jnp.where(first | second, 1.0, 0.0)
    earlier = jnp.where(iota((rows, rows), 0) < iota((rows, rows), 1), 1.0, 0.0).astype(BF)
    slot = jnp.where(named > 0, dot(named.astype(BF), earlier), NONE).astype(BF)
    slots[...] = slot
    spread, wanted = rows_of_experts(experts, False)
    pick = jnp.where(dot(spread, slot) == wanted, 1.0, 0.0).astype(BF)
    for copy in copies[1:]:
        copy.wait()
    scale = jnp.where(first, weight[0:1, :], 0.0) + jnp.where(second, weight[1:2, :], 0.0)
    high[...] = scale.astype(BF)
    low[...] = (scale - scale.astype(BF).astype(F32)).astype(BF)
    values = tok[...].astype(F32)
    mean = jnp.sum(values, axis=1, keepdims=True) * (1.0 / width)
    center = values - mean
    variance = jnp.sum(center * center, axis=1, keepdims=True) * (1.0 / width)
    columns = pl.ds(pl.multiple_of(sel[0] * quarter, quarter), quarter)
    part = tok[:, columns].astype(F32) - mean
    normed = (part * lax.rsqrt(variance + EPSILON) * gain[:, columns]).astype(BF)
    routed = dot(pick, normed).astype(BF)

    def write(at, value):
        message[:, at, :] = value

    packed(routed[: experts * MAIN], routed[experts * MAIN :], write)


def arrange_kernel(message, *outs):
    groups, parts = message.shape[0] // len(outs), message.shape[1] // CAP
    for number, out in enumerate(outs):
        here = slice(number * groups, (number + 1) * groups)

        def write(rows, columns, value):
            out[rows, columns] = value

        unpacked(lambda at: message[here, at, :], groups, parts, write)


def collect_kernel(*refs, count):
    message = refs[3 * count]
    groups = message.shape[0] // count
    for number in range(count):
        here = slice(number * groups, (number + 1) * groups)
        total = sum(r[...].astype(F32) for r in refs[3 * number : 3 * number + 3]).astype(BF)

        def write(at, value):
            message[here, at, :] = value

        packed(total[: groups * MAIN], total[groups * MAIN :], write)


def mixer_kernel(slots, high, low, mix_high, mix_low):
    spread, wanted = rows_of_experts(slots.shape[0], True)

    def of_rows(value):
        return lax.dot_general(value[...], spread, (((0,), (1,)), ((), ())), preferred_element_type=F32)

    named = of_rows(slots) == wanted
    for scale, mix in ((high, mix_high), (low, mix_low)):
        mix[...] = jnp.where(named, of_rows(scale), 0.0).astype(BF)


def combine_kernel(message, mix_high, mix_low, out, plain):
    def write(rows, columns, value):
        plain[rows, columns] = value

    unpacked(lambda at: message[:, at, :], message.shape[0], message.shape[1] // CAP, write)
    out[...] = (dot(mix_high[...], plain[...]) + dot(mix_low[...], plain[...])).astype(BF)


def stage_kernel(gate, up, down, both, out, sems):
    hidden = gate.shape[2]
    copies = [pltpu.make_async_copy(down.at[0], out, sems.at[0])]
    for j in range(hidden // LANES):
        for which, weight in ((0, gate), (1, up)):
            here = 2 * j + which
            copies.append(
                pltpu.make_async_copy(
                    weight.at[0, :, j * LANES : (j + 1) * LANES],
                    both.at[:, here * LANES : (here + 1) * LANES],
                    sems.at[1 + here],
                )
            )
    for copy in copies:
        copy.start()
    for copy in copies:
        copy.wait()


def expert_kernel(sel, *refs):
    pieces, (both_0, down_0, both_1, down_1), refs = refs[:4], refs[4:8], refs[8:]
    outs, (rows, hidden) = refs[:4], refs[4:]
    quarter = pieces[0].shape[1]
    width = down_0.shape[0]
    for k in range(4):
        rows[:, pl.ds(pl.multiple_of(sel[k] * quarter, quarter), quarter)] = pieces[k][...]
    for half, both in enumerate((both_0, both_1)):
        values = dot(rows[...], both[...])
        for j in range(width // LANES):
            gate = values[:, 2 * j * LANES : (2 * j + 1) * LANES]
            up = values[:, (2 * j + 1) * LANES : (2 * j + 2) * LANES]
            at = half * width + j * LANES
            hidden[:, at : at + LANES] = (gate / (1.0 + jnp.exp(-gate)) * up).astype(BF)
    for k in range(4):
        here = pl.ds(pl.multiple_of(sel[4 + k] * quarter, quarter), quarter)
        part = dot(hidden[:, :width], down_0[:, here]) + dot(hidden[:, width:], down_1[:, here])
        outs[k][...] = part.astype(BF)


def add_kernel(a, b, out):
    out[...] = (a[...].astype(F32) + b[...].astype(F32)).astype(BF)


def call(kernel, args, outs, scratch=(), spaces=None, limit=12, flops=1 << 28):
    spaces = spaces or [pltpu.VMEM] * len(args)
    args = [pltpu.with_memory_space_constraint(a, s) if s == pltpu.HBM else a for a, s in zip(args, spaces, strict=True)]
    return pl.pallas_call(
        kernel,
        in_specs=[whole(space) for space in spaces],
        out_specs=[whole()] * len(outs),
        out_shape=outs,
        scratch_shapes=scratch,
        compiler_params=pltpu.CompilerParams(vmem_limit_bytes=limit * MIB),
        cost_estimate=pl.CostEstimate(flops=flops, bytes_accessed=4 * MIB, transcendentals=0),
    )(*args)


def layer(tokens, norm_gain, expert_ids, route_weight, w_gate, w_up, w_down):
    tok_rows, width = tokens.shape
    experts = lax.axis_size("z") * lax.axis_size("y")
    across = lax.axis_size("x")
    quarter = width // across
    parts = quarter // LANES
    hidden = w_gate.shape[2]
    x = lax.axis_index("x")
    shape = jax.ShapeDtypeStruct
    dma = pltpu.SemaphoreType.DMA

    def shift(value, by):
        return lax.ppermute(value, "x", [(i, (i + by) % across) for i in range(across)])

    def exchange(value):
        return lax.all_to_all(value, ("z", "y"), 0, 0, tiled=True)

    near = [(x + by) % across for by in (0, 1, 3, 2)]
    sel = jnp.stack([near[k] for k in (0, 2, 1, 3, 0, 1, 2, 3)]).astype(jnp.int32)

    theirs = [lax.ppermute(w, "c", [(0, 1), (1, 0)]) for w in (w_gate, w_up, w_down)]
    message = shape((experts, parts * CAP, LANES), BF)
    table = shape((experts, tok_rows), BF)
    hbm = pltpu.HBM
    send, slots, high, low = call(
        prep_kernel,
        [sel, tokens, norm_gain.reshape(1, width), expert_ids.T, route_weight.T],
        [message, table, table, table],
        [
            pltpu.VMEM(tokens.shape, BF),
            pltpu.VMEM((1, width), F32),
            pltpu.VMEM(expert_ids.shape[::-1], jnp.int32),
            pltpu.VMEM(expert_ids.shape[::-1], F32),
            dma((4,)),
        ],
        spaces=[pltpu.SMEM, hbm, hbm, hbm, hbm],
    )
    arrived = exchange(send)
    weights = []
    for g, u, d in ((w_gate, w_up, w_down), theirs):
        weights += call(
            stage_kernel,
            [g, u, d],
            [pltpu.VMEM((width, 2 * hidden), BF), pltpu.VMEM((hidden, width), BF)],
            [dma((1 + 2 * hidden // LANES,))],
            spaces=[hbm] * 3,
            flops=1 << 31,
        )
    mix = shape((tok_rows, experts * CAP), BF)
    mixers = call(mixer_kernel, [slots, high, low], [mix, mix], flops=1 << 30)

    count = 2
    rows = experts * CAP // count
    piece = shape((rows, quarter), BF)
    chunks = call(arrange_kernel, [arrived], [piece] * count)
    sums = []
    for number, mine in enumerate(chunks):
        way = 1 if number % 2 == 0 else -1
        left = shift(mine, 1)
        right = shift(mine, -1)
        far = shift(left if way == 1 else right, way)
        outs = call(
            expert_kernel,
            [sel, mine, left, right, far, *weights],
            [piece] * 4,
            [pltpu.VMEM((rows, width), BF), pltpu.VMEM((rows, 2 * hidden), BF)],
            spaces=[pltpu.SMEM] + [pltpu.VMEM] * 8,
            limit=20,
            flops=12 * rows * width * hidden,
        )
        passed = shift(outs[3], way)
        near_by = 1 if way == 1 else 2
        direct = shift(outs[3 - near_by], -way)
        relay = call(add_kernel, [outs[near_by], passed], [piece])[0]
        sums += [outs[0], direct, shift(relay, way)]
    back = call(functools.partial(collect_kernel, count=count), sums, [message])[0]
    returned = exchange(back)
    return call(
        combine_kernel,
        [returned, *mixers],
        [shape((tok_rows, quarter), BF)],
        [pltpu.VMEM((experts * CAP, quarter), BF)],
    )[0]


def solution(mesh):
    finer = Mesh(mesh.devices.reshape(8, 4, 2, mesh.shape["tp"]), ("z", "y", "c", "x"))
    in_specs = (
        P(EP, None),
        P(),
        P(EP, None),
        P(EP, None),
        P(EP, None, "x"),
        P(EP, None, "x"),
        P(EP, "x", None),
    )
    return jax.shard_map(layer, mesh=finer, in_specs=in_specs, out_specs=P(EP, "x"), check_vma=False)
```

```python
import functools

import jax
import jax.numpy as jnp
from jax import lax
from jax.experimental import pallas as pl
from jax.experimental.pallas import tpu as pltpu
from jax.sharding import Mesh
from jax.sharding import PartitionSpec as P


EPSILON = 1e-05
EP = ("z", "y", "c")
CAP, MAIN, REST = 20, 16, 4
LANES = 128
NONE = -64.0
BF, F32 = jnp.bfloat16, jnp.float32
MIB = 1024 * 1024


dot = functools.partial(jnp.dot, preferred_element_type=F32)


def whole(space=pltpu.VMEM):
    return pl.BlockSpec(memory_space=space)


def iota(shape, dim):
    return lax.broadcasted_iota(jnp.int32, shape, dim)


def moved(groups, k, dtype=BF):
    plain = (REST * groups, MAIN * groups)
    group_of = iota(plain, 0) // REST == iota(plain, 1) // MAIN
    same = iota(plain, 1) % MAIN == iota(plain, 0) % REST + k * REST
    return jnp.where(group_of & same, 1.0, 0.0).astype(dtype)


def packed(main, rest, write):
    groups, parts = main.shape[0] // MAIN, main.shape[1] // LANES
    last = None
    for k in range(parts):
        here = slice(k * LANES, (k + 1) * LANES)
        write(slice(k * MAIN, (k + 1) * MAIN), main[:, here].reshape(groups, MAIN, LANES))
        term = lax.dot_general(moved(groups, k), rest[:, here], (((0,), (0,)), ((), ())), preferred_element_type=F32)
        last = term if last is None else last + term
    write(slice(parts * MAIN, parts * (MAIN + REST)), last.astype(BF).reshape(groups, MAIN, LANES))


def unpacked(read, groups, parts, write):
    last = read(slice(parts * MAIN, parts * (MAIN + REST))).reshape(groups * MAIN, LANES)
    for k in range(parts):
        here = slice(k * LANES, (k + 1) * LANES)
        write(slice(0, groups * MAIN), here, read(slice(k * MAIN, (k + 1) * MAIN)).reshape(groups * MAIN, LANES))
        write(slice(groups * MAIN, groups * CAP), here, dot(moved(groups, k), last).astype(BF))


def rows_of_experts(experts, flip):
    rows = experts * CAP
    row, expert = (iota((rows, experts), 0), iota((rows, experts), 1))
    first = experts * MAIN
    owner = jnp.where(row < first, row // MAIN, (row - first) // REST)
    spread = jnp.where(owner == expert, 1.0, 0.0).astype(BF)
    shape, dim = ((1, rows), 1) if flip else ((rows, 1), 0)
    at = iota(shape, dim)
    slot = jnp.where(at < first, at % MAIN, MAIN + (at - first) % REST).astype(F32)
    return spread, slot


def prep_kernel(sel, tokens, gain_hbm, ids_hbm, weight_hbm, message, slots, high, low, tok, gain, ids, weight, sems):
    copies = [
        pltpu.make_async_copy(source, target, sems.at[n])
        for n, (source, target) in enumerate(
            ((ids_hbm, ids), (tokens, tok), (gain_hbm, gain), (weight_hbm, weight))
        )
    ]
    for copy in copies:
        copy.start()
    rows, width = tok.shape
    experts = slots.shape[0]
    quarter = message.shape[1] // CAP * LANES
    copies[0].wait()
    number = iota((experts, rows), 0)
    first, second = number == ids[0:1, :], number == ids[1:2, :]
    named = jnp.where(first | second, 1.0, 0.0)
    earlier = jnp.where(iota((rows, rows), 0) < iota((rows, rows), 1), 1.0, 0.0).astype(BF)
    slot = jnp.where(named > 0, dot(named.astype(BF), earlier), NONE).astype(BF)
    slots[...] = slot
    spread, wanted = rows_of_experts(experts, False)
    pick = jnp.where(dot(spread, slot) == wanted, 1.0, 0.0).astype(BF)
    for copy in copies[1:]:
        copy.wait()
    scale = jnp.where(first, weight[0:1, :], 0.0) + jnp.where(second, weight[1:2, :], 0.0)
    high[...] = scale.astype(BF)
    low[...] = (scale - scale.astype(BF).astype(F32)).astype(BF)
    values = tok[...].astype(F32)
    mean = jnp.sum(values, axis=1, keepdims=True) * (1.0 / width)
    center = values - mean
    variance = jnp.sum(center * center, axis=1, keepdims=True) * (1.0 / width)
    columns = pl.ds(pl.multiple_of(sel[0] * quarter, quarter), quarter)
    part = tok[:, columns].astype(F32) - mean
    normed = (part * lax.rsqrt(variance + EPSILON) * gain[:, columns]).astype(BF)
    routed = dot(pick, normed).astype(BF)

    def write(at, value):
        message[:, at, :] = value

    packed(routed[: experts * MAIN], routed[experts * MAIN :], write)


def arrange_kernel(message, *outs):
    groups, parts = message.shape[0] // len(outs), message.shape[1] // CAP
    for number, out in enumerate(outs):
        here = slice(number * groups, (number + 1) * groups)

        def write(rows, columns, value):
            out[rows, columns] = value

        unpacked(lambda at: message[here, at, :], groups, parts, write)


def collect_kernel(own_0, own_1, relayed_0, direct_1, both, message):
    groups = message.shape[0] // 2
    rows = own_0.shape[0]
    terms = (own_0, relayed_0, both.at[rows:, :]), (own_1, direct_1, both.at[:rows, :])
    for number in range(2):
        here = slice(number * groups, (number + 1) * groups)
        total = sum(r[...].astype(F32) for r in terms[number]).astype(BF)

        def write(at, value):
            message[here, at, :] = value

        packed(total[: groups * MAIN], total[groups * MAIN :], write)


def mixer_kernel(slots, high, low, mix_high, mix_low):
    spread, wanted = rows_of_experts(slots.shape[0], True)

    def of_rows(value):
        return lax.dot_general(value[...], spread, (((0,), (1,)), ((), ())), preferred_element_type=F32)

    named = of_rows(slots) == wanted
    for scale, mix in ((high, mix_high), (low, mix_low)):
        mix[...] = jnp.where(named, of_rows(scale), 0.0).astype(BF)


def combine_kernel(message, mix_high, mix_low, out, plain):
    def write(rows, columns, value):
        plain[rows, columns] = value

    unpacked(lambda at: message[:, at, :], message.shape[0], message.shape[1] // CAP, write)
    out[...] = (dot(mix_high[...], plain[...]) + dot(mix_low[...], plain[...])).astype(BF)


def stage_kernel(gate, up, down, both, out, sems):
    hidden = gate.shape[2]
    copies = [pltpu.make_async_copy(down.at[0], out, sems.at[0])]
    for j in range(hidden // LANES):
        for which, weight in ((0, gate), (1, up)):
            here = 2 * j + which
            copies.append(
                pltpu.make_async_copy(
                    weight.at[0, :, j * LANES : (j + 1) * LANES],
                    both.at[:, here * LANES : (here + 1) * LANES],
                    sems.at[1 + here],
                )
            )
    for copy in copies:
        copy.start()
    for copy in copies:
        copy.wait()


def expert_kernel(sel, *refs):
    pieces, (both_0, down_0, both_1, down_1), refs = refs[:4], refs[4:8], refs[8:]
    outs, (rows, hidden) = refs[:4], refs[4:]
    quarter = pieces[0].shape[1]
    width = down_0.shape[0]
    for k in range(4):
        rows[:, pl.ds(pl.multiple_of(sel[k] * quarter, quarter), quarter)] = pieces[k][...]
    for half, both in enumerate((both_0, both_1)):
        values = dot(rows[...], both[...])
        for j in range(width // LANES):
            gate = values[:, 2 * j * LANES : (2 * j + 1) * LANES]
            up = values[:, (2 * j + 1) * LANES : (2 * j + 2) * LANES]
            at = half * width + j * LANES
            hidden[:, at : at + LANES] = (gate / (1.0 + jnp.exp(-gate)) * up).astype(BF)
    for k in range(4):
        here = pl.ds(pl.multiple_of(sel[4 + k] * quarter, quarter), quarter)
        part = dot(hidden[:, :width], down_0[:, here]) + dot(hidden[:, width:], down_1[:, here])
        outs[k][...] = part.astype(BF)


def add_kernel(a, b, *rest):
    *behind, out = rest
    rows = a.shape[0]
    out[:rows, :] = (a[...].astype(F32) + b[...].astype(F32)).astype(BF)
    for number, value in enumerate(behind):
        out[(number + 1) * rows : (number + 2) * rows, :] = value[...]


def call(kernel, args, outs, scratch=(), spaces=None, limit=12, flops=1 << 28):
    spaces = spaces or [pltpu.VMEM] * len(args)
    args = [pltpu.with_memory_space_constraint(a, s) if s == pltpu.HBM else a for a, s in zip(args, spaces, strict=True)]
    return pl.pallas_call(
        kernel,
        in_specs=[whole(space) for space in spaces],
        out_specs=[whole()] * len(outs),
        out_shape=outs,
        scratch_shapes=scratch,
        compiler_params=pltpu.CompilerParams(vmem_limit_bytes=limit * MIB),
        cost_estimate=pl.CostEstimate(flops=flops, bytes_accessed=4 * MIB, transcendentals=0),
    )(*args)


def layer(tokens, norm_gain, expert_ids, route_weight, w_gate, w_up, w_down):
    tok_rows, width = tokens.shape
    experts = lax.axis_size("z") * lax.axis_size("y")
    across = lax.axis_size("x")
    quarter = width // across
    parts = quarter // LANES
    hidden = w_gate.shape[2]
    x = lax.axis_index("x")
    shape = jax.ShapeDtypeStruct
    dma = pltpu.SemaphoreType.DMA

    def shift(value, by):
        return lax.ppermute(value, "x", [(i, (i + by) % across) for i in range(across)])

    def exchange(value):
        return lax.all_to_all(value, ("z", "y"), 0, 0, tiled=True)

    near = [(x + by) % across for by in (0, 1, 3, 2)]
    sel = jnp.stack([near[k] for k in (0, 2, 1, 3, 0, 1, 2, 3)]).astype(jnp.int32)

    theirs = [lax.ppermute(w, "c", [(0, 1), (1, 0)]) for w in (w_gate, w_up, w_down)]
    message = shape((experts, parts * CAP, LANES), BF)
    table = shape((experts, tok_rows), BF)
    hbm = pltpu.HBM
    send, slots, high, low = call(
        prep_kernel,
        [sel, tokens, norm_gain.reshape(1, width), expert_ids.T, route_weight.T],
        [message, table, table, table],
        [
            pltpu.VMEM(tokens.shape, BF),
            pltpu.VMEM((1, width), F32),
            pltpu.VMEM(expert_ids.shape[::-1], jnp.int32),
            pltpu.VMEM(expert_ids.shape[::-1], F32),
            dma((4,)),
        ],
        spaces=[pltpu.SMEM, hbm, hbm, hbm, hbm],
    )
    arrived = exchange(send)
    weights = []
    for g, u, d in ((w_gate, w_up, w_down), theirs):
        weights += call(
            stage_kernel,
            [g, u, d],
            [pltpu.VMEM((width, 2 * hidden), BF), pltpu.VMEM((hidden, width), BF)],
            [dma((1 + 2 * hidden // LANES,))],
            spaces=[hbm] * 3,
            flops=1 << 31,
        )
    mix = shape((tok_rows, experts * CAP), BF)
    mixers = call(mixer_kernel, [slots, high, low], [mix, mix], flops=1 << 30)

    count = 2
    rows = experts * CAP // count
    piece = shape((rows, quarter), BF)
    chunks = call(arrange_kernel, [arrived], [piece] * count)
    left_0, left_1 = (shift(chunks[n], 1) for n in range(count))
    right_0, right_1 = (shift(chunks[n], -1) for n in range(count))
    far_0, far_1 = shift(left_0, 1), shift(right_1, -1)

    def expert(*pieces):
        return call(
            expert_kernel,
            [sel, *pieces, *weights],
            [piece] * 4,
            [pltpu.VMEM((rows, width), BF), pltpu.VMEM((rows, 2 * hidden), BF)],
            spaces=[pltpu.SMEM] + [pltpu.VMEM] * 8,
            limit=20,
            flops=12 * rows * width * hidden,
        )

    own_1, next_1, last_1, far_1 = expert(chunks[1], left_1, right_1, far_1)
    passed_1 = shift(far_1, -1)
    direct_1 = shift(next_1, 1)
    own_0, next_0, last_0, far_0 = expert(chunks[0], left_0, right_0, far_0)
    passed_0 = shift(far_0, 1)
    twice = shape((2 * rows, quarter), BF)
    both = shift(call(add_kernel, [last_1, passed_1, last_0], [twice])[0], -1)
    relayed_0 = shift(call(add_kernel, [next_0, passed_0], [piece])[0], 1)
    back = call(collect_kernel, [own_0, own_1, relayed_0, direct_1, both], [message])[0]
    returned = exchange(back)
    return call(
        combine_kernel,
        [returned, *mixers],
        [shape((tok_rows, quarter), BF)],
        [pltpu.VMEM((experts * CAP, quarter), BF)],
    )[0]


def solution(mesh):
    finer = Mesh(mesh.devices.reshape(8, 4, 2, mesh.shape["tp"]), ("z", "y", "c", "x"))
    in_specs = (
        P(EP, None),
        P(),
        P(EP, None),
        P(EP, None),
        P(EP, None, "x"),
        P(EP, None, "x"),
        P(EP, "x", None),
    )
    return jax.shard_map(layer, mesh=finer, in_specs=in_specs, out_specs=P(EP, "x"), check_vma=False)
```

```python
import functools

import jax
import jax.numpy as jnp
from jax import lax
from jax.experimental import pallas as pl
from jax.experimental.pallas import tpu as pltpu
from jax.sharding import Mesh
from jax.sharding import PartitionSpec as P


EPSILON = 1e-05
EP = ("z", "y", "c")
CAP, MAIN, REST = 20, 16, 4
LANES = 128
PIECES = 4
NONE = -64.0
BF, F32 = jnp.bfloat16, jnp.float32
MIB = 1024 * 1024


dot = functools.partial(jnp.dot, preferred_element_type=F32)


def whole(space=pltpu.VMEM):
    return pl.BlockSpec(memory_space=space)


def iota(shape, dim):
    return lax.broadcasted_iota(jnp.int32, shape, dim)


def moved(groups, k, dtype=BF):
    plain = (REST * groups, MAIN * groups)
    group_of = iota(plain, 0) // REST == iota(plain, 1) // MAIN
    same = iota(plain, 1) % MAIN == iota(plain, 0) % REST + k * REST
    return jnp.where(group_of & same, 1.0, 0.0).astype(dtype)


def packed(main, rest, write):
    groups, parts = main.shape[0] // MAIN, main.shape[1] // LANES
    last = None
    for k in range(parts):
        here = slice(k * LANES, (k + 1) * LANES)
        write(slice(k * MAIN, (k + 1) * MAIN), main[:, here].reshape(groups, MAIN, LANES))
        term = lax.dot_general(moved(groups, k), rest[:, here], (((0,), (0,)), ((), ())), preferred_element_type=F32)
        last = term if last is None else last + term
    write(slice(parts * MAIN, parts * (MAIN + REST)), last.astype(BF).reshape(groups, MAIN, LANES))


def unpacked(read, groups, parts, write):
    last = read(slice(parts * MAIN, parts * (MAIN + REST))).reshape(groups * MAIN, LANES)
    for k in range(parts):
        here = slice(k * LANES, (k + 1) * LANES)
        write(slice(0, groups * MAIN), here, read(slice(k * MAIN, (k + 1) * MAIN)).reshape(groups * MAIN, LANES))
        write(slice(groups * MAIN, groups * CAP), here, dot(moved(groups, k), last).astype(BF))


def rows_of_experts(experts, flip):
    rows = experts * CAP
    row, expert = (iota((rows, experts), 0), iota((rows, experts), 1))
    first = experts * MAIN
    owner = jnp.where(row < first, row // MAIN, (row - first) // REST)
    spread = jnp.where(owner == expert, 1.0, 0.0).astype(BF)
    shape, dim = ((1, rows), 1) if flip else ((rows, 1), 0)
    at = iota(shape, dim)
    slot = jnp.where(at < first, at % MAIN, MAIN + (at - first) % REST).astype(F32)
    return spread, slot


def prep_kernel(sel, tokens, gain_hbm, ids_hbm, weight_hbm, message, slots, high, low, tok, gain, ids, weight, sems):
    copies = [
        pltpu.make_async_copy(source, target, sems.at[n])
        for n, (source, target) in enumerate(
            ((ids_hbm, ids), (tokens, tok), (gain_hbm, gain), (weight_hbm, weight))
        )
    ]
    for copy in copies:
        copy.start()
    rows, width = tok.shape
    experts = slots.shape[0]
    quarter = message.shape[1] // CAP * LANES
    copies[0].wait()
    number = iota((experts, rows), 0)
    first, second = number == ids[0:1, :], number == ids[1:2, :]
    named = jnp.where(first | second, 1.0, 0.0)
    earlier = jnp.where(iota((rows, rows), 0) < iota((rows, rows), 1), 1.0, 0.0).astype(BF)
    slot = jnp.where(named > 0, dot(named.astype(BF), earlier), NONE).astype(BF)
    slots[...] = slot
    spread, wanted = rows_of_experts(experts, False)
    pick = jnp.where(dot(spread, slot) == wanted, 1.0, 0.0).astype(BF)
    for copy in copies[1:]:
        copy.wait()
    scale = jnp.where(first, weight[0:1, :], 0.0) + jnp.where(second, weight[1:2, :], 0.0)
    high[...] = scale.astype(BF)
    low[...] = (scale - scale.astype(BF).astype(F32)).astype(BF)
    values = tok[...].astype(F32)
    mean = jnp.sum(values, axis=1, keepdims=True) * (1.0 / width)
    center = values - mean
    variance = jnp.sum(center * center, axis=1, keepdims=True) * (1.0 / width)
    columns = pl.ds(pl.multiple_of(sel[0] * quarter, quarter), quarter)
    part = tok[:, columns].astype(F32) - mean
    normed = (part * lax.rsqrt(variance + EPSILON) * gain[:, columns]).astype(BF)
    routed = dot(pick, normed).astype(BF)

    def write(at, value):
        message[:, at, :] = value

    packed(routed[: experts * MAIN], routed[experts * MAIN :], write)


def arrange_kernel(message, *outs):
    groups, parts = message.shape[0] // len(outs), message.shape[1] // CAP
    for number, out in enumerate(outs):
        here = slice(number * groups, (number + 1) * groups)

        def write(rows, columns, value):
            out[rows, columns] = value

        unpacked(lambda at: message[here, at, :], groups, parts, write)


def collect_kernel(own_0, own_1, relayed_a, relayed_b, direct_1, both, message):
    groups = message.shape[0] // 2
    rows = own_0.shape[0]
    relayed = jnp.concatenate([relayed_a[...].astype(F32), relayed_b[...].astype(F32)], axis=0)
    totals = [own_0[...].astype(F32) + relayed + both[rows:, :].astype(F32)]
    totals.append(own_1[...].astype(F32) + direct_1[...].astype(F32) + both[:rows, :].astype(F32))
    for number, total in enumerate(totals):
        here = slice(number * groups, (number + 1) * groups)
        total = total.astype(BF)

        def write(at, value):
            message[here, at, :] = value

        packed(total[: groups * MAIN], total[groups * MAIN :], write)


def mixer_kernel(slots, high, low, mix_high, mix_low):
    spread, wanted = rows_of_experts(slots.shape[0], True)

    def of_rows(value):
        return lax.dot_general(value[...], spread, (((0,), (1,)), ((), ())), preferred_element_type=F32)

    named = of_rows(slots) == wanted
    for scale, mix in ((high, mix_high), (low, mix_low)):
        mix[...] = jnp.where(named, of_rows(scale), 0.0).astype(BF)


def combine_kernel(message, mix_high, mix_low, out, plain):
    def write(rows, columns, value):
        plain[rows, columns] = value

    unpacked(lambda at: message[:, at, :], message.shape[0], message.shape[1] // CAP, write)
    out[...] = (dot(mix_high[...], plain[...]) + dot(mix_low[...], plain[...])).astype(BF)


def weight_parts(sel, gate, up, both):
    hidden, rows = gate.shape[2], gate.shape[1] // PIECES
    for n in range(PIECES):
        source, target = pl.ds(pl.multiple_of(sel[n] * rows, rows), rows), slice(n * rows, (n + 1) * rows)
        yield gate.at[0, source], both.at[target, :hidden]
        yield up.at[0, source], both.at[target, hidden:]


def staged(parts, sems):
    copies = [pltpu.make_async_copy(source, target, sems.at[n]) for n, (source, target) in enumerate(parts)]
    for copy in copies:
        copy.start()
    for copy in copies:
        copy.wait()


def stage_kernel(sel, gate, up, both, sems):
    staged(weight_parts(sel, gate, up, both), sems)


def stage_down_kernel(sel, gate, up, down_0, down_1, both, down, sems):
    parts = list(weight_parts(sel, gate, up, both))
    size = down_0.shape[1] // 2
    for number, source in enumerate((down_0, down_1)):
        for n in range(2):
            at = (2 * number + n) * size
            parts.append((source.at[0, n * size : (n + 1) * size], down.at[at : at + size]))
    staged(parts, sems)


def expert_kernel(sel, *refs):
    pieces, (both_0, both_1, down), refs = refs[:4], refs[4:7], refs[7:]
    outs, hidden = refs[:-1], refs[-1]
    quarter = pieces[0].shape[1]
    width = down.shape[0] // 2
    rows = jnp.concatenate([piece[...] for piece in pieces], axis=1)
    for half, both in enumerate((both_0, both_1)):
        values = dot(rows, both[...])
        for j in range(width // LANES):
            gate = values[:, j * LANES : (j + 1) * LANES]
            up = values[:, width + j * LANES : width + (j + 1) * LANES]
            at = half * width + j * LANES
            hidden[:, at : at + LANES] = (gate / (1.0 + jnp.exp(-gate)) * up).astype(BF)
    for k in range(4):
        here = pl.ds(pl.multiple_of(sel[4 + k] * quarter, quarter), quarter)
        part = dot(hidden[...], down[:, here])
        if k < 3:
            outs[k][...] = part.astype(BF)
    at = 0
    for out in outs[3:]:
        out[...] = part[at : at + out.shape[0]].astype(BF)
        at += out.shape[0]


def add_kernel(a, b, *rest):
    *behind, out = rest
    rows = a.shape[0]
    out[:rows, :] = (a[...].astype(F32) + b[...].astype(F32)).astype(BF)
    for number, value in enumerate(behind):
        out[(number + 1) * rows : (number + 2) * rows, :] = value[...]


def add_half_kernel(a, b, out, at):
    rows = out.shape[0]
    out[...] = (a[at * rows : (at + 1) * rows, :].astype(F32) + b[...].astype(F32)).astype(BF)


def call(kernel, args, outs, scratch=(), spaces=None, limit=12, flops=1 << 28):
    spaces = spaces or [pltpu.VMEM] * len(args)
    args = [pltpu.with_memory_space_constraint(a, s) if s == pltpu.HBM else a for a, s in zip(args, spaces, strict=True)]
    return pl.pallas_call(
        kernel,
        in_specs=[whole(space) for space in spaces],
        out_specs=[whole()] * len(outs),
        out_shape=outs,
        scratch_shapes=scratch,
        compiler_params=pltpu.CompilerParams(vmem_limit_bytes=limit * MIB),
        cost_estimate=pl.CostEstimate(flops=flops, bytes_accessed=4 * MIB, transcendentals=0),
    )(*args)


def layer(tokens, norm_gain, expert_ids, route_weight, w_gate, w_up, w_down):
    tok_rows, width = tokens.shape
    experts = lax.axis_size("z") * lax.axis_size("y")
    across = lax.axis_size("x")
    quarter = width // across
    parts = quarter // LANES
    hidden = w_gate.shape[2]
    x = lax.axis_index("x")
    shape = jax.ShapeDtypeStruct
    dma = pltpu.SemaphoreType.DMA

    def shift(value, by):
        return lax.ppermute(value, "x", [(i, (i + by) % across) for i in range(across)])

    def exchange(value):
        return lax.all_to_all(value, ("z", "y"), 0, 0, tiled=True)

    near = [(x + by) % across for by in (0, 1, 3, 2)]
    sel = jnp.stack([near[k] for k in (0, 2, 1, 3, 0, 1, 2, 3)]).astype(jnp.int32)

    theirs = [lax.ppermute(w, "c", [(0, 1), (1, 0)]) for w in (w_gate, w_up, w_down)]
    message = shape((experts, parts * CAP, LANES), BF)
    table = shape((experts, tok_rows), BF)
    hbm = pltpu.HBM
    send, slots, high, low = call(
        prep_kernel,
        [sel, tokens, norm_gain.reshape(1, width), expert_ids.T, route_weight.T],
        [message, table, table, table],
        [
            pltpu.VMEM(tokens.shape, BF),
            pltpu.VMEM((1, width), F32),
            pltpu.VMEM(expert_ids.shape[::-1], jnp.int32),
            pltpu.VMEM(expert_ids.shape[::-1], F32),
            dma((4,)),
        ],
        spaces=[pltpu.SMEM, hbm, hbm, hbm, hbm],
    )
    arrived = exchange(send)
    both, full = pltpu.VMEM((width, 2 * hidden), BF), pltpu.VMEM((2 * hidden, width), BF)
    ours = call(
        stage_kernel, [sel, w_gate, w_up], [both], [dma((2 * PIECES,))], spaces=[pltpu.SMEM] + [hbm] * 2, flops=1 << 31
    )
    others = call(
        stage_down_kernel,
        [sel, *theirs[:2], w_down, theirs[2]],
        [both, full],
        [dma((2 * PIECES + 4,))],
        spaces=[pltpu.SMEM] + [hbm] * 4,
        flops=1 << 31,
    )
    weights = [*ours, *others]
    mix = shape((tok_rows, experts * CAP), BF)
    mixers = call(mixer_kernel, [slots, high, low], [mix, mix], flops=1 << 30)

    count = 2
    rows = experts * CAP // count
    piece = shape((rows, quarter), BF)
    chunks = call(arrange_kernel, [arrived], [piece] * count)
    left_0, left_1 = (shift(chunks[n], 1) for n in range(count))
    right_0, right_1 = (shift(chunks[n], -1) for n in range(count))
    far_0, far_1 = shift(left_0, 1), shift(right_1, -1)

    half = shape((rows // 2, quarter), BF)

    def expert(number, *pieces):
        return call(
            expert_kernel,
            [sel, *pieces, *weights],
            [piece] * 3 + ([half, half] if number == 0 else [piece]),
            [pltpu.VMEM((rows, 2 * hidden), BF)],
            spaces=[pltpu.SMEM] + [pltpu.VMEM] * 7,
            limit=20,
            flops=12 * rows * width * hidden,
        )

    own_1, next_1, last_1, far_1 = expert(1, chunks[1], left_1, right_1, far_1)
    passed_1 = shift(far_1, -1)
    direct_1 = shift(next_1, 1)
    own_0, next_0, last_0, *far_0 = expert(0, chunks[0], left_0, right_0, far_0)
    passed_0 = [shift(f, 1) for f in far_0]
    twice = shape((2 * rows, quarter), BF)
    both = shift(call(add_kernel, [last_1, passed_1, last_0], [twice])[0], -1)
    relayed_0 = [
        shift(call(functools.partial(add_half_kernel, at=n), [next_0, p], [half])[0], 1)
        for n, p in enumerate(passed_0)
    ]
    back = call(collect_kernel, [own_0, own_1, *relayed_0, direct_1, both], [message])[0]
    returned = exchange(back)
    return call(
        combine_kernel,
        [returned, *mixers],
        [shape((tok_rows, quarter), BF)],
        [pltpu.VMEM((experts * CAP, quarter), BF)],
    )[0]


def solution(mesh):
    finer = Mesh(mesh.devices.reshape(8, 4, 2, mesh.shape["tp"]), ("z", "y", "c", "x"))
    in_specs = (
        P(EP, None),
        P(),
        P(EP, None),
        P(EP, None),
        P(EP, None, "x"),
        P(EP, None, "x"),
        P(EP, "x", None),
    )
    return jax.shard_map(layer, mesh=finer, in_specs=in_specs, out_specs=P(EP, "x"), check_vma=False)
```
